32 devices in a mesh: grp: 2 (over x), fs: 4 (over y, core), tp: 4 (over z).
Axes of the slice: x: 2, y: 2, z: 4, core: 2. Of those that a mesh axis runs over, the one named last changes fastest.
Arguments:
- stream: bfloat16 [4096, 2048], P(('grp', 'fs', 'tp')), parts along dimension 0, may hold values from -4 to 4
- gain_first: bfloat16 [2048], replicated, may hold values from 0.099609375 to 1.8984375
- gate_first: bfloat16 [2048, 4096], P('fs', 'tp'), may hold values from -0.125 to 0.125
- up_first: bfloat16 [2048, 4096], P('fs', 'tp'), may hold values from -0.125 to 0.125
- down_first: bfloat16 [4096, 2048], P('tp', 'fs'), may hold values from -0.09375 to 0.09375
- gain_second: bfloat16 [2048], replicated, may hold values from 0.099609375 to 1.8984375
- gate_second: bfloat16 [2048, 4096], P('fs', 'tp'), may hold values from -0.125 to 0.125
- up_second: bfloat16 [2048, 4096], P('fs', 'tp'), may hold values from -0.125 to 0.125
- down_second: bfloat16 [4096, 2048], P('tp', 'fs'), may hold values from -0.09375 to 0.09375
Outputs:
- result: bfloat16 [4096, 2048], P(('grp', 'fs', 'tp')), parts along dimension 0
The draws below stay inside these ranges and needn't reach their ends.
There are 2 independent parts, one for each index of `grp`. The reference program is written for one: setup_inputs(seed, part) draws one part's arguments, and reference() takes and returns one part's arrays. A program takes and returns all parts, laid end to end along the dimension named above; an argument that names none is the same for every part. Nothing has to cross between parts.
All inputs are finite; a program needn't handle non-finite values.
Results may differ from the reference program's by a relative error of at most 0.018.
Values may be sent and summed in bfloat16 or wider, within the bound.
A program may use at most 64 MiB of HBM per device.

```python
import jax
import jax.numpy as jnp
from jax import lax

D = 2048
FF = 4096
TOKENS = 2048
N_TP = 4


def block_scale(rng, extent, shards, smallest, largest):
    level = 1.0
    for position, blocks in shards:
        steps = jax.random.uniform(jax.random.fold_in(jax.random.fold_in(rng, 6), position), (blocks,), jnp.float32, smallest / len(shards), largest / len(shards))
        level = level * jnp.repeat(jnp.exp(steps), extent[position] // blocks).reshape((-1,) + (1,) * (len(extent) - 1 - position))
    return level


def scatter_about(stream_key, dims, deviation, bound, cuts=(), kind=jnp.bfloat16):
    drawn = deviation * jax.random.normal(stream_key, dims, jnp.float32)
    if cuts:
        drawn = drawn * block_scale(stream_key, dims, cuts, -0.22, 0.18)
    return jnp.clip(drawn, -bound, bound).astype(kind)


def setup_inputs(seed: int = 0, part: int = 0) -> dict:
    streams_of = jax.random.split(jax.random.key(seed), 10)
    part_keys = jax.random.split(jax.random.fold_in(streams_of[9], part), 10)
    return {
        "stream": scatter_about(part_keys[0], (TOKENS, D), 0.5, 4.0, ((0, 16),)),
        "gain_first": jnp.clip(1.0 + 0.18 * jax.random.normal(streams_of[1], (D,), jnp.float32), 0.099609375, 1.8984375).astype(jnp.bfloat16),
        "gate_first": scatter_about(streams_of[2], (D, FF), D ** -0.5, 0.125, ((0, 4), (1, 4))),
        "up_first": scatter_about(streams_of[3], (D, FF), D ** -0.5, 0.125, ((0, 4), (1, 4))),
        "down_first": scatter_about(streams_of[4], (FF, D), FF ** -0.5, 0.09375, ((0, 4), (1, 4))),
        "gain_second": jnp.clip(1.0 + 0.18 * jax.random.normal(streams_of[5], (D,), jnp.float32), 0.099609375, 1.8984375).astype(jnp.bfloat16),
        "gate_second": scatter_about(streams_of[6], (D, FF), D ** -0.5, 0.125, ((0, 4), (1, 4))),
        "up_second": scatter_about(streams_of[7], (D, FF), D ** -0.5, 0.125, ((0, 4), (1, 4))),
        "down_second": scatter_about(streams_of[8], (FF, D), FF ** -0.5, 0.09375, ((0, 4), (1, 4))),
    }


def half_branch(stream, gain, w_gate, w_up, w_down):
    stream_f = stream.astype(jnp.float32)
    normed = (stream_f * lax.rsqrt(lax.optimization_barrier(jnp.mean(stream_f * stream_f, axis=-1, keepdims=True)) + 1e-06) * gain.astype(jnp.float32)).astype(jnp.bfloat16)
    gate_act = jnp.dot(normed, w_gate, preferred_element_type=jnp.float32)
    up_act = jnp.dot(normed, w_up, preferred_element_type=jnp.float32)
    hidden = (jax.nn.silu(gate_act) * up_act).astype(jnp.bfloat16)
    span_width = FF // N_TP
    summed = jnp.zeros(stream.shape, jnp.float32)
    for shard in range(N_TP):
        partial_sum = jnp.dot(hidden[:, shard * span_width:(shard + 1) * span_width], w_down[shard * span_width:(shard + 1) * span_width], preferred_element_type=jnp.float32).astype(jnp.bfloat16)
        partial_sum = lax.optimization_barrier(partial_sum)
        summed = summed + partial_sum.astype(jnp.float32)
    return (stream_f + 0.5 * summed).astype(jnp.bfloat16)

def reference(stream, gain_first, gate_first, up_first, down_first, gain_second, gate_second, up_second, down_second):
    middle = half_branch(stream, gain_first, gate_first, up_first, down_first)
    return half_branch(middle, gain_second, gate_second, up_second, down_second)
```

```python
import functools

import jax
import jax.numpy as jnp
from jax import lax
from jax.experimental import pallas as pl
from jax.experimental.pallas import tpu as pltpu
from jax.sharding import PartitionSpec as P

MESH = pl.DeviceIdType.MESH
CORES = 2
VMEM_LIMIT = 60 * 1024 * 1024


def kernel(
    sizes,
    stream, gain_a, gain_b, gate_a, up_a, down_a, gate_b, up_b, down_b,
    out,
    gu, dn, xg, hid, part, rbuf, acc, mid,
    y_s, y_r, x_s, x_r, c_s, c_r, f_s, f_r, l_s, ag_s, ag_r, rs_s, rs_r,
):
    G, m, n, T, D, F, J = sizes
    Y = m // CORES
    C = D // J
    weights = (gate_a, up_a, down_a, gate_b, up_b, down_b)
    gains = (gain_a, gain_b)
    g = lax.axis_index("grp")
    fs = lax.axis_index("fs")
    me = lax.axis_index("tp")
    y = fs // CORES
    c = lax.rem(fs, CORES)
    mate = y * CORES + (CORES - 1 - c)
    right = lax.rem(me + 1, n)
    left = lax.rem(me + n - 1, n)

    def row_of(k):
        return lax.rem(y + k + Y, Y) * CORES + c

    def grp_of(i):
        return lax.rem(g + i + G, G)

    barrier = pltpu.get_barrier_semaphore()
    for k in range(1, Y):
        pl.semaphore_signal(barrier, inc=1, device_id={"fs": row_of(k)}, device_id_type=MESH)
    for i in range(1, G):
        pl.semaphore_signal(barrier, inc=1, device_id={"grp": grp_of(i)}, device_id_type=MESH)
    pl.semaphore_signal(barrier, inc=1, device_id={"fs": mate}, device_id_type=MESH)

    @pl.when(me < n - 1)
    def _():
        pl.semaphore_signal(barrier, inc=1, device_id={"tp": right}, device_id_type=MESH)

    @pl.when(me > 0)
    def _():
        pl.semaphore_signal(barrier, inc=1, device_id={"tp": left}, device_id_type=MESH)

    @pl.when(jnp.logical_and(me > 0, me < n - 1))
    def _():
        pl.semaphore_wait(barrier, Y - 1 + G - 1 + 1 + 2)

    @pl.when(jnp.logical_not(jnp.logical_and(me > 0, me < n - 1)))
    def _():
        pl.semaphore_wait(barrier, Y - 1 + G - 1 + 1 + 1)

    def rows_of(a):
        return weights[a].shape[0]

    def own(a, h=None):
        if h is None:
            return weights[a]
        half = rows_of(a) // G
        return weights[a].at[pl.ds(pl.multiple_of(h * half, half), half), :]

    def slot(a, j, h=None):
        b, t = a // 3, a % 3
        rows = rows_of(a)
        half = rows if h is None else rows // G
        off = 0 if h is None else h * half
        if t < 2:
            return gu.at[b, t, pl.ds(pl.multiple_of(j * rows + off, half), half), :]
        cols = D // m
        return dn.at[b, pl.ds(pl.multiple_of(off, half), half), pl.ds(pl.multiple_of(j * cols, cols), cols)]

    def remote(src, dst, ss, rs, dev):
        return pltpu.make_async_remote_copy(
            src_ref=src, dst_ref=dst, send_sem=ss, recv_sem=rs, device_id=dev, device_id_type=MESH
        )

    def local_copy(a):
        return pltpu.make_async_copy(own(a), slot(a, fs), l_s.at[a])

    def y_copy(a, k):
        return remote(own(a, g), slot(a, fs, g), y_s.at[a, k - 1], y_r.at[a, k - 1], {"fs": row_of(k)})

    def y_arrived(a, k):
        remote(own(a, g), slot(a, row_of(-k), g), y_s.at[a, k - 1], y_r.at[a, k - 1], {"fs": row_of(k)}).wait_recv()

    def c_copy(a):
        return remote(own(a), slot(a, fs), c_s.at[a], c_r.at[a], {"fs": mate})

    def c_arrived(a):
        remote(own(a), slot(a, mate), c_s.at[a], c_r.at[a], {"fs": mate}).wait_recv()

    def x_copy(a, k, i):
        where = slot(a, row_of(-k), g)
        return remote(where, where, x_s.at[a, k - 1, i - 1], x_r.at[a, k - 1, i - 1], {"grp": grp_of(i)})

    def x_arrived(a, k, i):
        where = slot(a, row_of(-k), grp_of(-i))
        remote(where, where, x_s.at[a, k - 1, i - 1], x_r.at[a, k - 1, i - 1], {"grp": grp_of(i)}).wait_recv()

    def f_copy(a, k, i):
        where = slot(a, row_of(-k), grp_of(-i))
        return remote(where, where, f_s.at[a, k - 1, i], f_r.at[a, k - 1, i], {"fs": mate})

    def f_arrived(a, k, i):
        row = lax.rem(y - k + Y, Y) * CORES + (CORES - 1 - c)
        where = slot(a, row, grp_of(-i))
        remote(where, where, f_s.at[a, k - 1, i], f_r.at[a, k - 1, i], {"fs": mate}).wait_recv()

    def y_event(a):
        for k in range(1, Y):
            y_arrived(a, k)
            for i in range(1, G):
                x_copy(a, k, i).start()
            f_copy(a, k, 0).start()

    def x_event(a):
        for k in range(1, Y):
            for i in range(1, G):
                x_arrived(a, k, i)
                f_copy(a, k, i).start()

    def complete(a):
        local_copy(a).wait()
        c_arrived(a)
        for k in range(1, Y):
            for i in range(G):
                f_arrived(a, k, i)

    def block(b, blk):
        return xg.at[b, pl.ds(pl.multiple_of(blk * T, T), T), :]

    def ag(b, way, blk):
        where = block(b, blk)
        return remote(where, where, ag_s.at[b, way, blk], ag_r.at[b, blk], {"tp": right if way == 0 else left})

    def ag_step(b, s, way, then=None):
        blk = me - s if way == 0 else me + s

        @pl.when(blk >= 0 if way == 0 else blk < n)
        def _():
            ag(b, way, blk).wait_recv()

            @pl.when(me < n - 1 if way == 0 else me > 0)
            def _():
                ag(b, way, blk).start()

            if then is not None:
                then(blk)

    def send_own(b):
        @pl.when(me < n - 1)
        def _():
            ag(b, 0, me).start()

        @pl.when(me > 0)
        def _():
            ag(b, 1, me).start()

    def normalize(b, source):
        step = min(32, T)

        @pl.loop(0, T // step)
        def _(r):
            rows = pl.ds(pl.multiple_of(r * step, step), step)
            v = source[rows, :].astype(jnp.float32)
            scale = lax.rsqrt(jnp.mean(v * v, axis=-1, keepdims=True) + 1e-06)
            dst = pl.ds(pl.multiple_of(me * T + r * step, step), step)
            xg[b, dst, :] = (v * scale * gains[b][...].astype(jnp.float32)).astype(jnp.bfloat16)

    tile = min(256, F)

    def hidden_of(b, blk):
        @pl.loop(0, F // tile)
        def _(q):
            cols = pl.ds(pl.multiple_of(q * tile, tile), tile)
            rows = pl.ds(pl.multiple_of(blk * T, T), T)
            x = xg[b, rows, :]
            gate = jnp.dot(x, gu[b, 0, :, cols], preferred_element_type=jnp.float32)
            up = jnp.dot(x, gu[b, 1, :, cols], preferred_element_type=jnp.float32)
            hid[rows, cols] = (gate / (1.0 + jnp.exp(-gate)) * up).astype(jnp.bfloat16)

    def rs(b, way, d, j):
        return remote(
            part.at[b, d, j], rbuf.at[b, way, d, j], rs_s.at[b, d, j], rs_r.at[b, way, d, j],
            {"tp": right if way == 0 else left},
        )

    def partial_of(b, blk):
        @pl.loop(0, J)
        def _(j):
            cols = pl.ds(pl.multiple_of(j * C, C), C)
            rows = pl.ds(pl.multiple_of(blk * T, T), T)
            part[b, blk, j] = jnp.dot(
                hid[rows, :], dn[b, :, cols], preferred_element_type=jnp.float32
            ).astype(jnp.bfloat16)

            @pl.when(jnp.logical_and(me == 0, blk > me))
            def _():
                rs(b, 0, blk, j).start()

            @pl.when(jnp.logical_and(me == n - 1, blk < me))
            def _():
                rs(b, 1, blk, j).start()

    def relay(b, q):
        @pl.loop(0, J)
        def _(j):
            for way, d, ok in (
                (0, q, jnp.logical_and(me > 0, q > me)),
                (1, n - 1 - q, jnp.logical_and(me < n - 1, n - 1 - q < me)),
            ):
                @pl.when(ok)
                def _():
                    rs(b, way, d, j).wait_recv()
                    part[b, d, j] = (
                        part[b, d, j].astype(jnp.float32) + rbuf[b, way, d, j].astype(jnp.float32)
                    ).astype(jnp.bfloat16)
                    rs(b, way, d, j).start()

    def finish(b, source, target):
        @pl.loop(0, J)
        def _(j):
            cols = pl.ds(pl.multiple_of(j * C, C), C)
            acc[...] = part[b, me, j].astype(jnp.float32)

            @pl.when(me > 0)
            def _():
                rs(b, 0, me, j).wait_recv()
                acc[...] += rbuf[b, 0, me, j].astype(jnp.float32)

            @pl.when(me < n - 1)
            def _():
                rs(b, 1, me, j).wait_recv()
                acc[...] += rbuf[b, 1, me, j].astype(jnp.float32)

            target[:, cols] = (source[:, cols].astype(jnp.float32) + 0.5 * acc[...]).astype(jnp.bfloat16)

    normalize(0, stream)
    send_own(0)
    for a in range(6):
        for k in range(1, Y):
            y_copy(a, k).start()
    for a in range(6):
        local_copy(a).start()
        c_copy(a).start()

    events = [("y", 0), ("y", 1), ("x", 0), ("y", 2), ("x", 1)]
    tail = [("x", 2), ("y", 3), ("x", 3), ("y", 4), ("x", 4), ("y", 5), ("x", 5)]

    def run(queue, count):
        for kind, a in queue[:count]:
            (y_event if kind == "y" else x_event)(a)
        del queue[:count]

    for s in range(1, n):
        ag_step(0, s, 0)
        ag_step(0, s, 1)
        run(events, 1 if s == 1 else 2)
    run(events, len(events))
    complete(0)
    complete(1)

    @pl.loop(0, n)
    def _(blk):
        hidden_of(0, blk)

    run(tail, 1)
    complete(2)

    @pl.loop(0, n)
    def _(blk):
        partial_of(0, blk)

    for q in range(1, n):
        run(tail, 2)
        relay(0, q)
    run(tail, len(tail))
    finish(0, stream, mid)
    normalize(1, mid)
    send_own(1)
    complete(3)
    complete(4)
    complete(5)

    def both(blk):
        hidden_of(1, blk)
        partial_of(1, blk)

    both(me)
    for s in range(1, n):
        ag_step(1, s, 0, both)
        ag_step(1, s, 1, both)
    for q in range(1, n):
        relay(1, q)
    finish(1, mid, out)

    for a in range(6):
        c_copy(a).wait_send()
        for k in range(1, Y):
            y_copy(a, k).wait_send()
            f_copy(a, k, 0).wait_send()
            for i in range(1, G):
                x_copy(a, k, i).wait_send()
                f_copy(a, k, i).wait_send()

    for b in range(2):
        @pl.loop(0, n)
        def _(d):
            @pl.when(jnp.logical_and(d <= me, me < n - 1))
            def _():
                ag(b, 0, d).wait_send()

            @pl.when(jnp.logical_and(d >= me, me > 0))
            def _():
                ag(b, 1, d).wait_send()

            @pl.loop(0, J)
            def _(j):
                @pl.when(d > me)
                def _():
                    rs(b, 0, d, j).wait_send()

                @pl.when(d < me)
                def _():
                    rs(b, 1, d, j).wait_send()


def local(sizes_of_mesh, stream, gain_a, gate_a, up_a, down_a, gain_b, gate_b, up_b, down_b):
    G, m, n = sizes_of_mesh
    T, D = stream.shape
    F = gate_a.shape[1]
    J = 4 if D % 512 == 0 else 1
    Y = m // CORES
    bf16 = jnp.bfloat16
    vmem = pl.BlockSpec(memory_space=pltpu.VMEM)
    anywhere = pl.BlockSpec(memory_space=pl.ANY)
    dma = pltpu.SemaphoreType.DMA
    return pl.pallas_call(
        functools.partial(kernel, (G, m, n, T, D, F, J)),
        out_shape=jax.ShapeDtypeStruct((T, D), bf16),
        in_specs=[vmem] * 3 + [anywhere] * 6,
        out_specs=vmem,
        scratch_shapes=[
            pltpu.VMEM((2, 2, D, F), bf16),
            pltpu.VMEM((2, F, D), bf16),
            pltpu.VMEM((2, n * T, D), bf16),
            pltpu.VMEM((n * T, F), bf16),
            pltpu.VMEM((2, n, J, T, D // J), bf16),
            pltpu.VMEM((2, 2, n, J, T, D // J), bf16),
            pltpu.VMEM((T, D // J), jnp.float32),
            pltpu.VMEM((T, D), bf16),
            dma((6, Y - 1)), dma((6, Y - 1)),
            dma((6, Y - 1, G - 1)), dma((6, Y - 1, G - 1)),
            dma((6,)), dma((6,)),
            dma((6, Y - 1, G)), dma((6, Y - 1, G)),
            dma((6,)),
            dma((2, 2, n)), dma((2, n)),
            dma((2, n, J)), dma((2, 2, n, J)),
        ],
        compiler_params=pltpu.CompilerParams(
            collective_id=0, has_side_effects=True, vmem_limit_bytes=VMEM_LIMIT
        ),
    )(
        stream, gain_a.reshape(1, D), gain_b.reshape(1, D),
        gate_a, up_a, down_a, gate_b, up_b, down_b,
    )


def solution(mesh):
    shape = mesh.shape
    in_specs = (
        P(("grp", "fs", "tp"), None),
        P(),
        P("fs", "tp"),
        P("fs", "tp"),
        P("tp", "fs"),
        P(),
        P("fs", "tp"),
        P("fs", "tp"),
        P("tp", "fs"),
    )
    out_specs = P(("grp", "fs", "tp"), None)
    body = functools.partial(local, (shape["grp"], shape["fs"], shape["tp"]))
    return jax.shard_map(body, mesh=mesh, in_specs=in_specs, out_specs=out_specs, check_vma=False)
```

```python
import functools

import jax
import jax.numpy as jnp
from jax import lax
from jax.experimental import pallas as pl
from jax.experimental.pallas import tpu as pltpu
from jax.sharding import PartitionSpec as P

MESH = pl.DeviceIdType.MESH
CORES = 2
PIECES = 2
VMEM_LIMIT = 60 * 1024 * 1024


def kernel(
    sizes,
    stream, gain_a, gain_b, gate_a, up_a, down_a, gate_b, up_b, down_b,
    out,
    gu, dn, xg, hid, part, rbuf, acc, mid,
    y_s, y_r, x_s, x_r, c_s, c_r, f_s, f_r, l_s, ag_s, ag_r, rs_s, rs_r,
):
    G, m, n, T, D, F, J = sizes
    Y = m // CORES
    C = D // J
    weights = (gate_a, up_a, down_a, gate_b, up_b, down_b)
    gains = (gain_a, gain_b)
    g = lax.axis_index("grp")
    fs = lax.axis_index("fs")
    me = lax.axis_index("tp")
    y = fs // CORES
    c = lax.rem(fs, CORES)
    mate = y * CORES + (CORES - 1 - c)
    right = lax.rem(me + 1, n)
    left = lax.rem(me + n - 1, n)

    def row_of(k):
        return lax.rem(y + k + Y, Y) * CORES + c

    def grp_of(i):
        return lax.rem(g + i + G, G)

    barrier = pltpu.get_barrier_semaphore()
    for k in range(1, Y):
        pl.semaphore_signal(barrier, inc=1, device_id={"fs": row_of(k)}, device_id_type=MESH)
    for i in range(1, G):
        pl.semaphore_signal(barrier, inc=1, device_id={"grp": grp_of(i)}, device_id_type=MESH)
    pl.semaphore_signal(barrier, inc=1, device_id={"fs": mate}, device_id_type=MESH)

    @pl.when(me < n - 1)
    def _():
        pl.semaphore_signal(barrier, inc=1, device_id={"tp": right}, device_id_type=MESH)

    @pl.when(me > 0)
    def _():
        pl.semaphore_signal(barrier, inc=1, device_id={"tp": left}, device_id_type=MESH)

    @pl.when(jnp.logical_and(me > 0, me < n - 1))
    def _():
        pl.semaphore_wait(barrier, Y - 1 + G - 1 + 1 + 2)

    @pl.when(jnp.logical_not(jnp.logical_and(me > 0, me < n - 1)))
    def _():
        pl.semaphore_wait(barrier, Y - 1 + G - 1 + 1 + 1)

    def rows_of(a):
        return weights[a].shape[0]

    def piece_rows(u, h):
        rows = rows_of(u // PIECES) // G
        sub = rows // PIECES
        return pl.multiple_of(h * rows + (u % PIECES) * sub, sub), sub

    def own(u, h):
        off, sub = piece_rows(u, h)
        return weights[u // PIECES].at[pl.ds(off, sub), :]

    def place(a, j, off, count):
        b, t = a // 3, a % 3
        if t < 2:
            return gu.at[b, t, pl.ds(pl.multiple_of(j * rows_of(a) + off, count), count), :]
        cols = D // m
        return dn.at[b, pl.ds(off, count), pl.ds(pl.multiple_of(j * cols, cols), cols)]

    def slot(u, j, h):
        off, sub = piece_rows(u, h)
        return place(u // PIECES, j, off, sub)

    def whole(a, j):
        return place(a, j, 0, rows_of(a))

    def remote(src, dst, ss, rs, dev):
        return pltpu.make_async_remote_copy(
            src_ref=src, dst_ref=dst, send_sem=ss, recv_sem=rs, device_id=dev, device_id_type=MESH
        )

    def local_copy(a):
        return pltpu.make_async_copy(weights[a], whole(a, fs), l_s.at[a])

    def y_copy(a, k):
        return remote(own(a, g), slot(a, fs, g), y_s.at[a, k - 1], y_r.at[a, k - 1], {"fs": row_of(k)})

    def y_arrived(a, k):
        remote(own(a, g), slot(a, row_of(-k), g), y_s.at[a, k - 1], y_r.at[a, k - 1], {"fs": row_of(k)}).wait_recv()

    def c_copy(a):
        return remote(weights[a], whole(a, fs), c_s.at[a], c_r.at[a], {"fs": mate})

    def c_arrived(a):
        remote(weights[a], whole(a, mate), c_s.at[a], c_r.at[a], {"fs": mate}).wait_recv()

    def x_copy(a, k, i):
        where = slot(a, row_of(-k), g)
        return remote(where, where, x_s.at[a, k - 1, i - 1], x_r.at[a, k - 1, i - 1], {"grp": grp_of(i)})

    def x_arrived(a, k, i):
        where = slot(a, row_of(-k), grp_of(-i))
        remote(where, where, x_s.at[a, k - 1, i - 1], x_r.at[a, k - 1, i - 1], {"grp": grp_of(i)}).wait_recv()

    def f_copy(a, k, i):
        where = slot(a, row_of(-k), grp_of(-i))
        return remote(where, where, f_s.at[a, k - 1, i], f_r.at[a, k - 1, i], {"fs": mate})

    def f_arrived(a, k, i):
        row = lax.rem(y - k + Y, Y) * CORES + (CORES - 1 - c)
        where = slot(a, row, grp_of(-i))
        remote(where, where, f_s.at[a, k - 1, i], f_r.at[a, k - 1, i], {"fs": mate}).wait_recv()

    def y_event(a):
        for k in range(1, Y):
            y_arrived(a, k)
            for i in range(1, G):
                x_copy(a, k, i).start()
            f_copy(a, k, 0).start()

    def x_event(a):
        for k in range(1, Y):
            for i in range(1, G):
                x_arrived(a, k, i)
                f_copy(a, k, i).start()

    def complete(a):
        local_copy(a).wait()
        c_arrived(a)
        for u in range(a * PIECES, (a + 1) * PIECES):
            for k in range(1, Y):
                for i in range(G):
                    f_arrived(u, k, i)

    def block(b, blk):
        return xg.at[b, pl.ds(pl.multiple_of(blk * T, T), T), :]

    def ag(b, way, blk):
        where = block(b, blk)
        return remote(where, where, ag_s.at[b, way, blk], ag_r.at[b, blk], {"tp": right if way == 0 else left})

    def ag_step(b, s, way, then=None):
        blk = me - s if way == 0 else me + s

        @pl.when(blk >= 0 if way == 0 else blk < n)
        def _():
            ag(b, way, blk).wait_recv()

            @pl.when(me < n - 1 if way == 0 else me > 0)
            def _():
                ag(b, way, blk).start()

            if then is not None:
                then(blk)

    def send_own(b):
        @pl.when(me < n - 1)
        def _():
            ag(b, 0, me).start()

        @pl.when(me > 0)
        def _():
            ag(b, 1, me).start()

    def normalize(b, source):
        step = min(32, T)

        @pl.loop(0, T // step)
        def _(r):
            rows = pl.ds(pl.multiple_of(r * step, step), step)
            v = source[rows, :].astype(jnp.float32)
            scale = lax.rsqrt(jnp.mean(v * v, axis=-1, keepdims=True) + 1e-06)
            dst = pl.ds(pl.multiple_of(me * T + r * step, step), step)
            xg[b, dst, :] = (v * scale * gains[b][...].astype(jnp.float32)).astype(jnp.bfloat16)

    tile = min(256, F)

    def hidden_of(b, blk):
        @pl.loop(0, F // tile)
        def _(q):
            cols = pl.ds(pl.multiple_of(q * tile, tile), tile)
            rows = pl.ds(pl.multiple_of(blk * T, T), T)
            x = xg[b, rows, :]
            gate = jnp.dot(x, gu[b, 0, :, cols], preferred_element_type=jnp.float32)
            up = jnp.dot(x, gu[b, 1, :, cols], preferred_element_type=jnp.float32)
            hid[rows, cols] = (gate / (1.0 + jnp.exp(-gate)) * up).astype(jnp.bfloat16)

    def rs(b, way, d, j):
        return remote(
            part.at[b, d, j], rbuf.at[b, way, d, j], rs_s.at[b, d, j], rs_r.at[b, way, d, j],
            {"tp": right if way == 0 else left},
        )

    def chunk_of(b, blk, j):
        cols = pl.ds(pl.multiple_of(j * C, C), C)
        rows = pl.ds(pl.multiple_of(blk * T, T), T)
        part[b, blk, j] = jnp.dot(
            hid[rows, :], dn[b, :, cols], preferred_element_type=jnp.float32
        ).astype(jnp.bfloat16)

        @pl.when(jnp.logical_and(me == 0, blk > me))
        def _():
            rs(b, 0, blk, j).start()

        @pl.when(jnp.logical_and(me == n - 1, blk < me))
        def _():
            rs(b, 1, blk, j).start()

    def partial_of(b, blk):
        @pl.loop(0, J)
        def _(j):
            chunk_of(b, blk, j)

    def relay(b, j, to_right, to_left):
        for way, d, ok in (
            (0, to_right, jnp.logical_and(me > 0, to_right > me)),
            (1, to_left, jnp.logical_and(me < n - 1, to_left < me)),
        ):
            @pl.when(ok)
            def _():
                rs(b, way, d, j).wait_recv()
                part[b, d, j] = (
                    part[b, d, j].astype(jnp.float32) + rbuf[b, way, d, j].astype(jnp.float32)
                ).astype(jnp.bfloat16)
                rs(b, way, d, j).start()

    def finish(b, source, target):
        @pl.loop(0, J)
        def _(j):
            cols = pl.ds(pl.multiple_of(j * C, C), C)
            acc[...] = part[b, me, j].astype(jnp.float32)

            @pl.when(me > 0)
            def _():
                rs(b, 0, me, j).wait_recv()
                acc[...] += rbuf[b, 0, me, j].astype(jnp.float32)

            @pl.when(me < n - 1)
            def _():
                rs(b, 1, me, j).wait_recv()
                acc[...] += rbuf[b, 1, me, j].astype(jnp.float32)

            target[:, cols] = (source[:, cols].astype(jnp.float32) + 0.5 * acc[...]).astype(jnp.bfloat16)

    for u in range(6 * PIECES):
        for k in range(1, Y):
            y_copy(u, k).start()
    normalize(0, stream)
    send_own(0)
    for a in range(6):
        local_copy(a).start()
        c_copy(a).start()

    events = [("y", 0)]
    for u in range(1, 6 * PIECES):
        events += [("y", u), ("x", u - 1)]
    events += [("x", 6 * PIECES - 1)]

    def run(last=None, count=0):
        stop = events.index(last) + 1 if last in events else (0 if last else min(count, len(events)))
        for kind, u in events[:stop]:
            (y_event if kind == "y" else x_event)(u)
        del events[:stop]

    def hidden_pair(b, first, last):
        @pl.loop(first, last)
        def _(s):
            for blk, ok in ((me - s, me - s >= 0), (me + s, me + s < n)):
                @pl.when(ok)
                def _():
                    hidden_of(b, blk)

    run(("x", 0))
    for s in range(1, n - 1):
        ag_step(0, s, 0)
        ag_step(0, s, 1)
        if s == 1:
            run(("x", 2 * PIECES - 2))
    run(("x", 2 * PIECES - 1))
    complete(0)
    complete(1)
    hidden_of(0, me)
    hidden_pair(0, 1, min(2, n - 1))
    run(("x", 3 * PIECES - 2))
    ag_step(0, n - 1, 0)
    ag_step(0, n - 1, 1)
    hidden_pair(0, min(2, n - 1), n)
    run(("x", 3 * PIECES - 1))
    complete(2)
    upper = lax.div(me, (n + 1) // 2)
    for j in range(J):
        @pl.loop(0, n)
        def _(t):
            chunk_of(0, t + (1 - upper) * (n - 1 - 2 * t), j)

        @pl.loop(1, n)
        def _(q):
            relay(0, j, n - q, q - 1)

        if j < J - 1:
            run(None, 4)
    run(None, len(events))
    finish(0, stream, mid)
    normalize(1, mid)
    send_own(1)
    complete(3)
    complete(4)
    complete(5)

    def both(blk):
        hidden_of(1, blk)
        partial_of(1, blk)

    both(me)
    for s in range(1, n):
        ag_step(1, s, 0, both)
        ag_step(1, s, 1, both)
    for q in range(1, n):
        @pl.loop(0, J)
        def _(j):
            relay(1, j, q, n - 1 - q)

    finish(1, mid, out)

    for a in range(6):
        c_copy(a).wait_send()
    for u in range(6 * PIECES):
        for k in range(1, Y):
            y_copy(u, k).wait_send()
            f_copy(u, k, 0).wait_send()
            for i in range(1, G):
                x_copy(u, k, i).wait_send()
                f_copy(u, k, i).wait_send()

    for b in range(2):
        @pl.loop(0, n)
        def _(d):
            @pl.when(jnp.logical_and(d <= me, me < n - 1))
            def _():
                ag(b, 0, d).wait_send()

            @pl.when(jnp.logical_and(d >= me, me > 0))
            def _():
                ag(b, 1, d).wait_send()

            @pl.loop(0, J)
            def _(j):
                @pl.when(d > me)
                def _():
                    rs(b, 0, d, j).wait_send()

                @pl.when(d < me)
                def _():
                    rs(b, 1, d, j).wait_send()


def local(sizes_of_mesh, stream, gain_a, gate_a, up_a, down_a, gain_b, gate_b, up_b, down_b):
    G, m, n = sizes_of_mesh
    T, D = stream.shape
    F = gate_a.shape[1]
    J = 4 if D % 512 == 0 else 1
    Y = m // CORES
    U = 6 * PIECES
    bf16 = jnp.bfloat16
    vmem = pl.BlockSpec(memory_space=pltpu.VMEM)
    anywhere = pl.BlockSpec(memory_space=pl.ANY)
    dma = pltpu.SemaphoreType.DMA
    return pl.pallas_call(
        functools.partial(kernel, (G, m, n, T, D, F, J)),
        out_shape=jax.ShapeDtypeStruct((T, D), bf16),
        in_specs=[vmem] * 3 + [anywhere] * 6,
        out_specs=vmem,
        scratch_shapes=[
            pltpu.VMEM((2, 2, D, F), bf16),
            pltpu.VMEM((2, F, D), bf16),
            pltpu.VMEM((2, n * T, D), bf16),
            pltpu.VMEM((n * T, F), bf16),
            pltpu.VMEM((2, n, J, T, D // J), bf16),
            pltpu.VMEM((2, 2, n, J, T, D // J), bf16),
            pltpu.VMEM((T, D // J), jnp.float32),
            pltpu.VMEM((T, D), bf16),
            dma((U, Y - 1)), dma((U, Y - 1)),
            dma((U, Y - 1, G - 1)), dma((U, Y - 1, G - 1)),
            dma((6,)), dma((6,)),
            dma((U, Y - 1, G)), dma((U, Y - 1, G)),
            dma((6,)),
            dma((2, 2, n)), dma((2, n)),
            dma((2, n, J)), dma((2, 2, n, J)),
        ],
        compiler_params=pltpu.CompilerParams(
            collective_id=0, has_side_effects=True, vmem_limit_bytes=VMEM_LIMIT
        ),
    )(
        stream, gain_a.reshape(1, D), gain_b.reshape(1, D),
        gate_a, up_a, down_a, gate_b, up_b, down_b,
    )


def solution(mesh):
    shape = mesh.shape
    in_specs = (
        P(("grp", "fs", "tp"), None),
        P(),
        P("fs", "tp"),
        P("fs", "tp"),
        P("tp", "fs"),
        P(),
        P("fs", "tp"),
        P("fs", "tp"),
        P("tp", "fs"),
    )
    out_specs = P(("grp", "fs", "tp"), None)
    body = functools.partial(local, (shape["grp"], shape["fs"], shape["tp"]))
    return jax.shard_map(body, mesh=mesh, in_specs=in_specs, out_specs=out_specs, check_vma=False)
```
